32 devices in a mesh: ep: 4 (over y, x), tp: 8 (over z, core).
Axes of the slice: x: 2, y: 2, z: 4, core: 2. Of those that a mesh axis runs over, the one named last changes fastest.
Arguments:
- hidden_in: bfloat16 [128, 4096], P('ep'), may hold values from -6 to 6
- mix_gain: float32 [4096], replicated, may hold values from 0.1 to 1.9
- w_query: bfloat16 [4096, 2048], P('ep', 'tp'), may hold values from -0.09375 to 0.09375
- w_key: bfloat16 [4096, 2048], P('ep', 'tp'), may hold values from -0.09375 to 0.09375
- w_value: bfloat16 [4096, 2048], P('ep', 'tp'), may hold values from -0.09375 to 0.09375
- w_outgate: bfloat16 [4096, 2048], P('ep', 'tp'), may hold values from -0.09375 to 0.09375
- w_gates: bfloat16 [2, 4096, 32], P(None, None, 'tp'), may hold values from -0.09375 to 0.09375
- gate_bias: float32 [2, 32], P(None, 'tp'), may hold values from -1 to 4
- state_matrix: float32 [128, 32, 64, 64], P('ep', 'tp'), may hold values from -2 to 2
- state_norm: float32 [128, 32, 64], P('ep', 'tp'), may hold values from -2 to 2
- state_max: float32 [128, 32], P('ep', 'tp'), may hold values from -3 to 3
- w_mix_out: bfloat16 [2048, 4096], P('tp'), may hold values from -0.125 to 0.125
- ffn_gain: float32 [4096], replicated, may hold values from 0.1 to 1.9
- routes: int32 [128, 2], replicated, may hold values from 0 to 7, all different within a row; in each aligned block of 32 rows (0 to 31, 32 to 63, ...) at most 9 rows name the same one
- route_weights: float32 [128, 2], P('ep'), may hold values from 0.1 to 1
- expert_gate: bfloat16 [8, 4096, 2048], P('ep', None, 'tp'), may hold values from -0.09375 to 0.09375
- expert_up: bfloat16 [8, 4096, 2048], P('ep', None, 'tp'), may hold values from -0.09375 to 0.09375
- expert_down: bfloat16 [8, 2048, 4096], P('ep', 'tp'), may hold values from -0.125 to 0.125
- shared_gate: bfloat16 [4096, 1024], P(None, 'tp'), may hold values from -0.09375 to 0.09375
- shared_up: bfloat16 [4096, 1024], P(None, 'tp'), may hold values from -0.09375 to 0.09375
- shared_down: bfloat16 [1024, 4096], P('tp'), may hold values from -0.1875 to 0.1875
Outputs:
- result: bfloat16 [128, 4096], P('ep', 'tp')
- new_matrix: float32 [128, 32, 64, 64], P('ep', 'tp')
- new_norm: float32 [128, 32, 64], P('ep', 'tp')
- new_max: float32 [128, 32], P('ep', 'tp')
The draws below stay inside these ranges and needn't reach their ends.
Inputs may be any that keep to these rules, and one draw needn't show every extreme that they name: `routes`: each row names 2 different experts. In each aligned block of 32 rows (the rows of one device group along ep) no expert is named by more than 9 rows, a bound that some block reaches.
All inputs are finite; a program needn't handle non-finite values.
Results may differ from the reference program's by a relative error of at most 0.023.
Values may be sent and summed in bfloat16 or wider, within the bound.
A program may use at most 64 MiB of HBM per device.

```python
import math
import jax
import jax.numpy as jnp
import numpy as np
from jax import lax

D = 4096
HEADS = 32
HEAD_DIM = 64
EXPERT_WIDTH = 2048
SHARED_WIDTH = 1024
TOP = 2
SEQ_GRP = 32
M_WIDTH = 2048
EXPERTS = 8
CAP = 9
BATCH = 128
N_EP = 4
N_TP = 8


def block_scale(own_key, shape, cuts, least, top_value):
    gain = 1.0
    for axis_at, parts in cuts:
        heights = jax.random.uniform(jax.random.fold_in(jax.random.fold_in(own_key, 6), axis_at), (parts,), jnp.float32, least / len(cuts), top_value / len(cuts))
        gain = gain * jnp.repeat(jnp.exp(heights), shape[axis_at] // parts).reshape((-1,) + (1,) * (len(shape) - 1 - axis_at))
    return gain


def deal_out(key, own, number, rows, count, top, most, skew):
    sequence = jax.random.permutation(key, count)
    packed, ordinary = portions_of(count, rows * top, most, skew, True), portions_of(count, rows * top, most, skew, False)
    places = jnp.arange(count)

    def named(lengths, rotation):
        used = int((lengths > 0).sum())
        fixed = max(1, used // 4)
        shifted = fixed + (places - fixed + rotation * (used - fixed)) % max(1, count - fixed)
        return jnp.zeros((count,), jnp.int32).at[sequence[jnp.where(places < fixed, places, shifted)]].set(jnp.asarray(lengths, jnp.int32))

    lengths = jnp.where(number % 4 == 0, named(packed, number // 4), named(ordinary, number - number // 4 - 1))
    mixed = jax.random.permutation(jax.random.fold_in(own, 3), count)
    source_of, receiver = mixed[0:count // 2 * 2:2], mixed[1:count // 2 * 2:2]
    room = jnp.minimum(lengths[source_of] - 1, most - lengths[receiver]) // 2
    room = jnp.where((source_of == sequence[0]) | (receiver == sequence[0]) | (lengths[receiver] == 0), 0, jnp.maximum(room, 0))
    shifted = jax.random.randint(jax.random.fold_in(own, 4), (count // 2,), 0, 1 << 20) % (room + 1)
    lengths = lengths.at[source_of].add(-shifted).at[receiver].add(shifted)
    items = jnp.searchsorted(jnp.cumsum(lengths), jnp.arange(rows * top), side="right").astype(jnp.int32)
    table = items.reshape(top, rows).T
    table = table[jax.random.permutation(jax.random.fold_in(own, 1), rows)]
    rotation = jax.random.randint(jax.random.fold_in(own, 2), (rows, 1), 0, top)
    return jnp.take_along_axis(table, (jnp.arange(top)[None, :] + rotation) % top, axis=1)


def portions_of(number_of, total, reach, lean, full):
    portions = [(1 << 20) // math.isqrt(standing ** lean) + 1 for standing in range(1, number_of + 1)]
    largest = reach if full else min(reach, max(-(-total // number_of), total * portions[0] // sum(portions)))
    least = 1 if total - largest >= number_of - 1 else 0
    holding, surplus = [largest] + [least] * (number_of - 1), total - largest - least * (number_of - 1)
    while surplus > 0:
        movable = [i for i in range(1, number_of) if holding[i] < largest] or [i for i in range(1, number_of) if holding[i] < reach]
        pool, left = sum([portions[i] for i in movable]), surplus
        for i in movable:
            addition = min(reach - holding[i], max(1, left * portions[i] // pool), surplus)
            holding[i] = holding[i] + addition
            surplus = surplus - addition
    return np.array(holding)


def bell_draw(rng, extent, scale, reach, cuts=(), kind=jnp.bfloat16):
    level = block_scale(rng, extent, cuts, -0.22, 0.18) if cuts else 1.0
    values = jax.random.normal(rng, extent, jnp.float32) * scale * level
    return jnp.minimum(jnp.maximum(values, -reach), reach).astype(kind)


def setup_inputs(seed: int = 0) -> dict:
    streams_of = jax.random.split(jax.random.key(seed), 22)
    hidden_in = bell_draw(streams_of[0], (BATCH, D), 1.0, 6.0, ((0, 4),))
    mix_gain = jnp.clip(1.0 + 0.18 * jax.random.normal(streams_of[1], (D,), jnp.float32), 0.1, 1.9)
    w_query = bell_draw(streams_of[2], (D, M_WIDTH), D ** -0.5, 0.09375, ((0, 4), (1, 8)))
    w_key = bell_draw(streams_of[3], (D, M_WIDTH), D ** -0.5, 0.09375, ((0, 4), (1, 8)))
    w_value = bell_draw(streams_of[4], (D, M_WIDTH), D ** -0.5, 0.09375, ((0, 4), (1, 8)))
    w_outgate = bell_draw(streams_of[5], (D, M_WIDTH), D ** -0.5, 0.09375, ((0, 4), (1, 8)))
    w_gates = bell_draw(streams_of[6], (2, D, HEADS), D ** -0.5, 0.09375, ((2, 8),))
    gate_bias = jnp.clip(-1.0 + 5.0 * jax.random.uniform(streams_of[7], (2, HEADS), jnp.float32) ** block_scale(streams_of[7], (2, HEADS), ((1, 8),), -0.2, 0.2), -1.0, 4.0)
    state_matrix = bell_draw(streams_of[8], (BATCH, HEADS, HEAD_DIM, HEAD_DIM), 0.15, 2.0, ((0, 4), (1, 8)), jnp.float32)
    state_norm = bell_draw(streams_of[9], (BATCH, HEADS, HEAD_DIM), 0.15, 2.0, ((0, 4), (1, 8)), jnp.float32)
    state_max = jnp.clip(jax.random.uniform(streams_of[10], (BATCH, HEADS), jnp.float32, -3.0, 3.0) * block_scale(streams_of[10], (BATCH, HEADS), ((0, 4), (1, 8)), -0.4, 0.0), -3.0, 3.0)
    w_mix_out = bell_draw(streams_of[11], (M_WIDTH, D), M_WIDTH ** -0.5, 0.125, ((0, 8),))
    ffn_gain = jnp.clip(1.0 + 0.18 * jax.random.normal(streams_of[12], (D,), jnp.float32), 0.1, 1.9)
    routes_keys = jax.random.split(jax.random.fold_in(streams_of[13], 1), BATCH // SEQ_GRP)
    routes_turns = jax.random.permutation(jax.random.fold_in(streams_of[13], 3), BATCH // SEQ_GRP)
    routes = jax.vmap(lambda own, number: deal_out(jax.random.fold_in(streams_of[13], 2), own, number, SEQ_GRP, EXPERTS, TOP, CAP, 2))(routes_keys, routes_turns).reshape((BATCH, TOP))
    route_weights = jnp.clip(jnp.exp(math.log(1.0) - 2.3025851 * jax.random.uniform(streams_of[14], (BATCH, TOP), jnp.float32) ** block_scale(streams_of[14], (BATCH, TOP), ((0, 4),), -0.2, 0.2)), 0.1, 1.0)
    expert_gate = bell_draw(streams_of[15], (EXPERTS, D, EXPERT_WIDTH), D ** -0.5, 0.09375, ((0, 4), (2, 8)))
    expert_up = bell_draw(streams_of[16], (EXPERTS, D, EXPERT_WIDTH), D ** -0.5, 0.09375, ((0, 4), (2, 8)))
    expert_down = bell_draw(streams_of[17], (EXPERTS, EXPERT_WIDTH, D), EXPERT_WIDTH ** -0.5, 0.125, ((0, 4), (1, 8)))
    shared_gate = bell_draw(streams_of[18], (D, SHARED_WIDTH), D ** -0.5, 0.09375, ((1, 8),))
    shared_up = bell_draw(streams_of[19], (D, SHARED_WIDTH), D ** -0.5, 0.09375, ((1, 8),))
    shared_down = bell_draw(streams_of[20], (SHARED_WIDTH, D), SHARED_WIDTH ** -0.5, 0.1875, ((0, 8),))
    return dict(hidden_in=hidden_in, mix_gain=mix_gain, w_query=w_query, w_key=w_key, w_value=w_value, w_outgate=w_outgate, w_gates=w_gates, gate_bias=gate_bias, state_matrix=state_matrix, state_norm=state_norm, state_max=state_max, w_mix_out=w_mix_out, ffn_gain=ffn_gain, routes=routes, route_weights=route_weights, expert_gate=expert_gate, expert_up=expert_up, expert_down=expert_down, shared_gate=shared_gate, shared_up=shared_up, shared_down=shared_down)


norm_eps = 1e-06

def rms_scale(inputs, scales):
    floats = inputs.astype(jnp.float32)
    return floats * lax.rsqrt(lax.optimization_barrier(jnp.mean(floats * floats, -1, keepdims=True)) + norm_eps) * scales

def block_sum(hidden, down_weight):
    row_count = hidden.shape[0]
    unit_count = hidden.shape[1]
    hidden_blocks = hidden.astype(jnp.float32).reshape(row_count, N_TP, unit_count // N_TP)
    down_blocks = down_weight.astype(jnp.float32).reshape(N_TP, unit_count // N_TP, down_weight.shape[1])
    partial_value = jnp.einsum('rpf,pfd->prd', hidden_blocks, down_blocks).astype(jnp.bfloat16)
    return lax.optimization_barrier(jnp.sum(partial_value.astype(jnp.float32), 0))

def reference(hidden_in, mix_gain, w_query, w_key, w_value, w_outgate, w_gates, gate_bias, state_matrix, state_norm, state_max, w_mix_out, ffn_gain, routes, route_weights, expert_gate, expert_up, expert_down, shared_gate, shared_up, shared_down):
    normed = rms_scale(hidden_in, mix_gain).astype(jnp.bfloat16)

    def project(weight):
        rounded = jnp.dot(normed, weight, preferred_element_type=jnp.float32).astype(jnp.bfloat16)
        rounded = lax.optimization_barrier(rounded)
        return rounded.astype(jnp.float32).reshape(BATCH, HEADS, HEAD_DIM)
    query_heads = project(w_query)
    key_heads = project(w_key) * HEAD_DIM ** (-0.5)
    value_heads = project(w_value)
    out_gate = project(w_outgate)
    gate_pre = jnp.einsum('sd,gdh->gsh', normed.astype(jnp.float32), w_gates.astype(jnp.float32))
    gate_pre = gate_pre + gate_bias[:, None, :]
    carried = jax.nn.log_sigmoid(gate_pre[1]) + state_max
    new_max = jnp.maximum(carried, gate_pre[0])
    forget_weight = jnp.exp(carried - new_max)[..., None]
    input_weight = jnp.exp(gate_pre[0] - new_max)[..., None]
    new_norm = forget_weight * state_norm + input_weight * key_heads
    new_matrix = forget_weight[..., None] * state_matrix + (input_weight * value_heads)[..., :, None] * key_heads[..., None, :]
    numerator = jnp.einsum('shek,shk->she', new_matrix, query_heads, precision=lax.Precision.HIGHEST)
    denominator = jnp.maximum(jnp.abs(lax.optimization_barrier(jnp.sum(new_norm * query_heads, -1))), 1.0)
    gated_out = (jax.nn.sigmoid(out_gate) * numerator / denominator[..., None]).reshape(BATCH, M_WIDTH)
    gated_out = gated_out.astype(jnp.bfloat16)
    stream = (hidden_in.astype(jnp.float32) + jnp.dot(gated_out, w_mix_out, preferred_element_type=jnp.float32)).astype(jnp.bfloat16)
    ffn_in = rms_scale(stream, ffn_gain).astype(jnp.bfloat16)
    shared_hidden = (jax.nn.silu(jnp.dot(ffn_in, shared_gate, preferred_element_type=jnp.float32)) * jnp.dot(ffn_in, shared_up, preferred_element_type=jnp.float32)).astype(jnp.bfloat16)
    shared_out = block_sum(shared_hidden, shared_down)
    grouped = routes.reshape(N_EP, SEQ_GRP * TOP)
    onehot = (grouped[..., None] == jnp.arange(EXPERTS, dtype=jnp.int32)[None, None, :]).astype(jnp.int32)
    earlier = jnp.cumsum(onehot, 1) - onehot
    rank_counts = lax.optimization_barrier(jnp.sum(earlier * onehot, -1))
    group_ids = jnp.arange(N_EP, dtype=jnp.int32)[:, None]
    slot_ids = (grouped * (N_EP * CAP) + group_ids * CAP + rank_counts).reshape(-1).astype(jnp.int32)
    token_ids = (jnp.arange(BATCH * TOP, dtype=jnp.int32) // TOP).astype(jnp.int32)
    slot_tokens = jnp.full((EXPERTS * N_EP * CAP,), BATCH, jnp.int32).at[slot_ids].set(token_ids)
    padded_in = jnp.concatenate([ffn_in, jnp.zeros((1, D), jnp.bfloat16)], 0)

    def run_expert(operands):
        slot_picks, gate_weight, up_weight, down_weight = operands
        rows_in = padded_in[slot_picks]
        hidden = (jax.nn.silu(jnp.dot(rows_in, gate_weight, preferred_element_type=jnp.float32)) * jnp.dot(rows_in, up_weight, preferred_element_type=jnp.float32)).astype(jnp.bfloat16)
        return block_sum(hidden, down_weight).astype(jnp.bfloat16)
    expert_rows = lax.map(run_expert, (slot_tokens.reshape(EXPERTS, N_EP * CAP), expert_gate, expert_up, expert_down))
    flat_rows = expert_rows.reshape(EXPERTS * N_EP * CAP, D)
    picked = flat_rows[slot_ids].astype(jnp.float32).reshape(BATCH, TOP, D)
    routed = lax.optimization_barrier(jnp.sum(route_weights[..., None] * picked, 1))
    result = (stream.astype(jnp.float32) + shared_out + routed).astype(jnp.bfloat16)
    return (result, new_matrix, new_norm, new_max)
```

```python
import functools

import jax
import jax.numpy as jnp
from jax import lax
from jax.experimental import pallas as pl
from jax.experimental.pallas import tpu as pltpu
from jax.sharding import PartitionSpec as P

norm_eps = 1e-06
F32 = jnp.float32
BF16 = jnp.bfloat16
MESH = pl.DeviceIdType.MESH


def dot(a, b):
    return jnp.dot(a, b, preferred_element_type=F32)


def layer_kernel(
    dims,
    hidden_ref,
    mix_gain_ref,
    w_gates_ref,
    bias_ref,
    norm_ref,
    max_ref,
    ffn_gain_ref,
    routes_ref,
    weights_ref,
    wq_hbm,
    wk_hbm,
    wv_hbm,
    wo_hbm,
    state_hbm,
    mix_hbm,
    sg_hbm,
    su_hbm,
    sd_hbm,
    eg_hbm,
    eu_hbm,
    ed_hbm,
    result_ref,
    new_max_ref,
    new_norm_ref,
    forget_ref,
    iv_ref,
    kk_ref,
    wq,
    wk,
    wv,
    wo,
    state,
    mix,
    sg,
    su,
    sd,
    eg,
    eu,
    ed,
    normed,
    gathered,
    part,
    proj_in,
    q_heads,
    pads,
    routes_t,
    mix_out,
    mix_in,
    mix_own,
    zs,
    zr,
    half,
    other,
    sel,
    rx_a,
    rx_b,
    x_shared,
    sh_out,
    sh_in,
    sh_own,
    x_rows,
    hid,
    pair_out,
    pair_in,
    pair_own,
    ret_out,
    ret_in,
    comb,
    zs2,
    zr2,
    local_sem,
    send_sem,
    recv_sem,
):
    E, T, S, D, H, hd, Le, cap, pad_rows, top = dims
    Z = T // 2
    SW = D // T
    Dk = D // E
    rows = Le * cap
    g = lax.axis_index("ep")
    t = lax.axis_index("tp")
    z = lax.div(t, 2)
    c = lax.rem(t, 2)
    partner = {"tp": t + 1 - 2 * c}
    locals_ = []
    for n, (src, dst) in enumerate(
        zip(
            (wq_hbm, wk_hbm, wv_hbm, wo_hbm, state_hbm, mix_hbm, sg_hbm, su_hbm, sd_hbm, eg_hbm, eu_hbm, ed_hbm),
            (wq, wk, wv, wo, state, mix, sg, su, sd, eg, eu, ed),
        )
    ):
        copy = pltpu.make_async_copy(src, dst, local_sem.at[n])
        copy.start()
        locals_.append(copy)

    barrier = pltpu.get_barrier_semaphore()
    lo = rows // 16 * 16
    if lo < pad_rows:
        for buf in (rx_a, rx_b, ret_in):
            buf[:, lo:, :] = jnp.zeros((E, pad_rows - lo, Z * SW), BF16)
    pl.semaphore_signal(barrier, inc=1, device_id=partner, device_id_type=MESH)
    for d in range(1, Z):
        pl.semaphore_signal(barrier, inc=1, device_id={"tp": lax.rem(z + d, Z) * 2 + c}, device_id_type=MESH)
    for d in range(1, E):
        pl.semaphore_signal(barrier, inc=1, device_id={"ep": lax.rem(g + d, E)}, device_id_type=MESH)

    sent = []

    def remote(src, dst, device):
        n = len(sent)
        copy = pltpu.make_async_remote_copy(
            src_ref=src,
            dst_ref=dst,
            send_sem=send_sem.at[n],
            recv_sem=recv_sem.at[n],
            device_id=device,
            device_id_type=MESH,
        )
        copy.start()
        sent.append(copy)
        return copy

    def ep_to(d):
        return lax.rem(g + d, E)

    def ep_from(d):
        return lax.rem(g + E - d, E)

    def z_to(d):
        return lax.rem(z + d, Z)

    def z_from(d):
        return lax.rem(z + Z - d, Z)

    def columns(zi, core):
        return pl.ds(pl.multiple_of((zi * 2 + core) * SW, SW), SW)

    def transposed(slot, value):
        pads[slot] = jnp.zeros((8, 128), F32)
        pads[slot, : value.shape[0], : value.shape[1]] = value
        return pads[slot].T

    floats = hidden_ref[...].astype(F32)
    scale = lax.rsqrt(jnp.mean(floats * floats, -1, keepdims=True) + norm_eps)
    for p in range(E):
        span = slice(p * Dk, (p + 1) * Dk)
        normed[p] = (hidden_ref[:, span].astype(F32) * scale * mix_gain_ref[:, span]).astype(BF16)
    pl.semaphore_wait(barrier, Z + E - 1)
    moves = [remote(normed.at[ep_to(d)], gathered.at[g], {"ep": ep_to(d)}) for d in range(1, E)]
    gathered[g] = normed[g]

    bias_t = transposed(0, bias_ref[...])
    gate_pre = []
    for role in range(2):
        total = jnp.zeros((H, S), F32)
        for p in range(E):
            total = total + lax.dot_general(
                w_gates_ref[role, :, p * Dk : (p + 1) * Dk],
                normed[p],
                (((1,), (1,)), ((), ())),
                preferred_element_type=F32,
            )
        gate_pre.append(total + bias_t[:H, role : role + 1])
    carried = jnp.minimum(gate_pre[1], 0.0) - jnp.log(1.0 + jnp.exp(-jnp.abs(gate_pre[1]))) + max_ref[...]
    new_max = jnp.maximum(carried, gate_pre[0])
    forget = jnp.exp(carried - new_max)
    take = jnp.exp(gate_pre[0] - new_max)
    new_max_ref[...] = new_max
    forget_ref[...] = forget
    forget_t = transposed(1, forget)
    take_t = transposed(2, take)

    route_floats = routes_ref[...].astype(F32)
    routes_t[...] = jnp.concatenate(
        [route_floats, jnp.zeros((8 - top, route_floats.shape[1]), F32)], 0
    ).T
    own_routes = routes_t[pl.ds(pl.multiple_of(g * S, 8), S), :]
    weights_t = transposed(3, weights_ref[...])
    lane = lax.broadcasted_iota(jnp.int32, (S, 128), 1).astype(F32)
    named = [(own_routes[:, k : k + 1] == lane).astype(F32) for k in range(top)]
    onehot = functools.reduce(jnp.add, named)
    earlier = (
        lax.broadcasted_iota(jnp.int32, (S, S), 0) > lax.broadcasted_iota(jnp.int32, (S, S), 1)
    ).astype(F32)
    rank = dot(earlier.astype(BF16), onehot.astype(BF16))
    owner = jnp.floor((lane + 0.5) / Le)
    base = rank + owner * pad_rows + (lane - owner * Le) * cap
    slot_lane = lax.broadcasted_iota(jnp.int32, (S, E * pad_rows), 1).astype(F32)
    match = jnp.zeros((S, E * pad_rows), F32)
    share = jnp.zeros((S, E * pad_rows), F32)
    for k in range(top):
        slot = jnp.sum(base * named[k], -1, keepdims=True)
        hit = slot_lane == slot
        match = jnp.where(hit, 1.0, match)
        share = jnp.where(hit, weights_t[:S, k : k + 1], share)
    chooser = match.T.astype(BF16)
    share_hi = share.astype(BF16)
    share_lo = (share - share_hi.astype(F32)).astype(BF16)

    for n in range(4):
        locals_[n].wait()
    for move in moves:
        move.wait_recv()
    stacked = gathered[...].reshape(E * S, Dk)
    hc = H * hd
    for n, weight in enumerate((wq, wk, wv, wo)):
        part[:, :, n * hc : (n + 1) * hc] = dot(stacked, weight[...]).astype(BF16).reshape(E, S, hc)
    moves = [remote(part.at[ep_to(d)], proj_in.at[g], {"ep": ep_to(d)}) for d in range(1, E)]
    locals_[4].wait()
    for move in moves:
        move.wait_recv()
    projected = part[g].astype(F32)
    for d in range(1, E):
        projected = projected + proj_in[ep_from(d)].astype(F32)
    projected = projected.astype(BF16).astype(F32)

    for h in range(H):
        q_heads[h] = projected[:, h * hd : (h + 1) * hd]
    lane64 = lax.broadcasted_iota(jnp.int32, (hd, 128), 1)

    def read_row(s, totals):
        out = []
        for h in range(H):
            product = state[s, h] * q_heads[h, pl.ds(s, 1), :]
            out.append(jnp.where(lane64 == s, jnp.sum(product, -1, keepdims=True), totals[h]))
        return tuple(out)

    reads = lax.fori_loop(0, S, read_row, tuple(jnp.zeros((hd, 128), F32) for _ in range(H)))
    gated = []
    for h in range(H):
        query = q_heads[h]
        key = projected[:, hc + h * hd : hc + (h + 1) * hd] * hd ** (-0.5)
        value = projected[:, 2 * hc + h * hd : 2 * hc + (h + 1) * hd]
        gate = projected[:, 3 * hc + h * hd : 3 * hc + (h + 1) * hd]
        keep = forget_t[:S, h : h + 1]
        put = take_t[:S, h : h + 1]
        put_value = put * value
        new_norm = keep * norm_ref[:, h, :] + put * key
        new_norm_ref[:, h, :] = new_norm
        iv_ref[:, h, :] = put_value
        kk_ref[:, h, :] = key
        numerator = keep * reads[h].T[:S, :] + put_value * jnp.sum(key * query, -1, keepdims=True)
        denominator = jnp.maximum(jnp.abs(jnp.sum(new_norm * query, -1, keepdims=True)), 1.0)
        gated.append(numerator / (denominator * (1.0 + jnp.exp(-gate))))
    gated = jnp.concatenate(gated, -1).astype(BF16)

    locals_[5].wait()
    moves = []
    for zi in range(Z):
        mix_out[zi] = dot(gated, mix[:, columns(zi, 1 - c)]).astype(BF16)
        moves.append(remote(mix_out.at[zi], mix_in.at[zi], partner))
    for zi in range(Z):
        mix_own[zi] = dot(gated, mix[:, columns(zi, c)])
    for move in moves:
        move.wait_recv()
    moves = []
    for d in range(1, Z):
        to = z_to(d)
        zs[to] = (mix_own[to] + mix_in[to].astype(F32)).astype(BF16)
        moves.append(remote(zs.at[to], zr.at[z], {"tp": to * 2 + c}))
    mixed = hidden_ref[:, columns(z, c)].astype(F32) + mix_own[z] + mix_in[z].astype(F32)
    for d in range(1, Z):
        moves[d - 1].wait_recv()
        mixed = mixed + zr[z_from(d)].astype(F32)
    stream_own = mixed.astype(BF16)

    half[z] = stream_own
    moves = [remote(half.at[z], half.at[z], {"tp": z_to(d) * 2 + c}) for d in range(1, Z)]
    shares = [remote(half.at[z], other.at[z], partner)]
    for d in range(1, Z):
        moves[d - 1].wait_recv()
        shares.append(remote(half.at[z_from(d)], other.at[z_from(d)], partner))
    for zi in range(Z):
        sel[:, :, zi * SW : (zi + 1) * SW] = dot(chooser, half[zi]).astype(BF16).reshape(E, pad_rows, SW)
    kept = pl.ds(0, -(-rows // 8) * 8)
    moves = [
        remote(sel.at[ep_to(d), kept], rx_a.at[g, kept], {"ep": ep_to(d)}) for d in range(1, E)
    ]
    rows_shares = [remote(sel.at[g, kept], rx_b.at[g, kept], partner)]
    rx_a[g] = sel[g]

    for move in shares:
        move.wait_recv()
    squares = jnp.zeros((S, 1), F32)
    for zi in range(Z):
        for buf in (half, other):
            floats = buf[zi].astype(F32)
            squares = squares + jnp.sum(floats * floats, -1, keepdims=True)
    scale = lax.rsqrt(squares / D + norm_eps)
    for zi in range(Z):
        for buf, core in ((half, c), (other, 1 - c)):
            span = columns(zi, core)
            x_shared[:, span] = (buf[zi].astype(F32) * scale * ffn_gain_ref[:, span]).astype(BF16)
    for n in range(6, 9):
        locals_[n].wait()
    inputs = x_shared[...]
    gate = dot(inputs, sg[...])
    shared_hidden = (gate / (1.0 + jnp.exp(-gate)) * dot(inputs, su[...])).astype(BF16)
    shared_moves = []
    for zi in range(Z):
        sh_out[zi] = dot(shared_hidden, sd[:, columns(zi, 1 - c)]).astype(BF16)
        shared_moves.append(remote(sh_out.at[zi], sh_in.at[zi], partner))
    for zi in range(Z):
        sh_own[zi] = dot(shared_hidden, sd[:, columns(zi, c)])

    for d in range(1, E):
        moves[d - 1].wait_recv()
        rows_shares.append(remote(rx_a.at[ep_from(d), kept], rx_b.at[ep_from(d), kept], partner))
    for move in rows_shares:
        move.wait_recv()
    count = E * pad_rows
    squares = jnp.zeros((count, 1), F32)
    for buf in (rx_a, rx_b):
        for zi in range(Z):
            floats = buf[:, :, zi * SW : (zi + 1) * SW].reshape(count, SW).astype(F32)
            squares = squares + jnp.sum(floats * floats, -1, keepdims=True)
    scale = lax.rsqrt(squares / D + norm_eps)
    for zi in range(Z):
        for buf, core in ((rx_a, c), (rx_b, 1 - c)):
            span = columns(zi, core)
            floats = buf[:, :, zi * SW : (zi + 1) * SW].reshape(count, SW).astype(F32)
            x_rows[:, span] = (floats * scale * ffn_gain_ref[:, span]).astype(BF16)
    for n in range(9, 12):
        locals_[n].wait()
    width = eg.shape[2]
    place = lax.broadcasted_iota(jnp.int32, (E, pad_rows, width), 1).reshape(count, width)
    for e in range(Le):
        gate = dot(x_rows[...], eg[e])
        value = gate / (1.0 + jnp.exp(-gate)) * dot(x_rows[...], eu[e])
        value = jnp.where((place >= e * cap) & (place < (e + 1) * cap), value, 0.0)
        hid[:, e * width : (e + 1) * width] = value.astype(BF16)
    pair_moves = []
    for zi in range(Z):
        pair_out[zi] = dot(hid[...], ed[:, columns(zi, 1 - c)]).astype(BF16)
        pair_moves.append(remote(pair_out.at[zi], pair_in.at[zi], partner))
    for zi in range(Z):
        pair_own[zi] = dot(hid[...], ed[:, columns(zi, c)])
    for zi in range(Z):
        pair_moves[zi].wait_recv()
        both = pair_own[zi] + pair_in[zi].astype(F32)
        ret_out[:, :, zi * SW : (zi + 1) * SW] = both.astype(BF16).reshape(E, pad_rows, SW)
    moves = [
        remote(ret_out.at[ep_to(d), kept], ret_in.at[g, kept], {"ep": ep_to(d)})
        for d in range(1, E)
    ]
    ret_in[g] = ret_out[g]
    for move in shared_moves:
        move.wait_recv()
    for move in moves:
        move.wait_recv()

    for zi in range(Z):
        back = ret_in[:, :, zi * SW : (zi + 1) * SW].reshape(count, SW)
        comb[zi] = dot(share_hi, back) + dot(share_lo, back) + sh_own[zi] + sh_in[zi].astype(F32)
    moves = []
    for d in range(1, Z):
        to = z_to(d)
        zs2[to] = comb[to].astype(BF16)
        moves.append(remote(zs2.at[to], zr2.at[z], {"tp": to * 2 + c}))
    total = half[z].astype(F32) + comb[z]
    for d in range(1, Z):
        moves[d - 1].wait_recv()
        total = total + zr2[z_from(d)].astype(F32)
    result_ref[...] = total.astype(BF16)
    for copy in sent:
        copy.wait_send()


def per_device(
    hidden_in,
    mix_gain,
    w_query,
    w_key,
    w_value,
    w_outgate,
    w_gates,
    gate_bias,
    state_matrix,
    state_norm,
    state_max,
    w_mix_out,
    ffn_gain,
    routes,
    route_weights,
    expert_gate,
    expert_up,
    expert_down,
    shared_gate,
    shared_up,
    shared_down,
):
    E = lax.axis_size("ep")
    T = lax.axis_size("tp")
    S, D = hidden_in.shape
    H, hd = state_matrix.shape[1:3]
    top = routes.shape[1]
    Le, _, width = expert_gate.shape
    cap = max(2, S * top // (Le * E) + 1)
    pad_rows = -(-Le * cap // 16) * 16
    Z, SW, Dk, count = T // 2, D // T, D // E, E * pad_rows
    batch = routes.shape[0]
    dims = (E, T, S, D, H, hd, Le, cap, pad_rows, top)
    vmem = pl.BlockSpec(memory_space=pltpu.VMEM)
    hbm = pl.BlockSpec(memory_space=pl.ANY)
    down = expert_down.reshape(Le * width, D)
    big = (
        w_query, w_key, w_value, w_outgate, state_matrix, w_mix_out,
        shared_gate, shared_up, shared_down, expert_gate, expert_up, down,
    )
    V = pltpu.VMEM
    sems = 6 * E + 8 * Z + 8
    result, new_max, new_norm, forget, iv, kk = pl.pallas_call(
        functools.partial(layer_kernel, dims),
        out_shape=(
            jax.ShapeDtypeStruct((S, SW), BF16),
            jax.ShapeDtypeStruct((H, S), F32),
            jax.ShapeDtypeStruct((S, H, hd), F32),
            jax.ShapeDtypeStruct((H, S), F32),
            jax.ShapeDtypeStruct((S, H, hd), F32),
            jax.ShapeDtypeStruct((S, H, hd), F32),
        ),
        in_specs=[vmem] * 9 + [hbm] * len(big),
        out_specs=(vmem,) * 6,
        scratch_shapes=[V(a.shape, a.dtype) for a in big]
        + [
            V((E, S, Dk), BF16),
            V((E, S, Dk), BF16),
            V((E, S, 4 * H * hd), BF16),
            V((E, S, 4 * H * hd), BF16),
            V((H, S, hd), F32),
            V((4, 8, 128), F32),
            V((batch, 8), F32),
            V((Z, S, SW), BF16),
            V((Z, S, SW), BF16),
            V((Z, S, SW), F32),
            V((Z, S, SW), BF16),
            V((Z, S, SW), BF16),
            V((Z, S, SW), BF16),
            V((Z, S, SW), BF16),
            V((E, pad_rows, Z * SW), BF16),
            V((E, pad_rows, Z * SW), BF16),
            V((E, pad_rows, Z * SW), BF16),
            V((S, D), BF16),
            V((Z, S, SW), BF16),
            V((Z, S, SW), BF16),
            V((Z, S, SW), F32),
            V((count, D), BF16),
            V((count, Le * width), BF16),
            V((Z, count, SW), BF16),
            V((Z, count, SW), BF16),
            V((Z, count, SW), F32),
            V((E, pad_rows, Z * SW), BF16),
            V((E, pad_rows, Z * SW), BF16),
            V((Z, S, SW), F32),
            V((Z, S, SW), BF16),
            V((Z, S, SW), BF16),
            pltpu.SemaphoreType.DMA((len(big),)),
            pltpu.SemaphoreType.DMA((sems,)),
            pltpu.SemaphoreType.DMA((sems,)),
        ],
        compiler_params=pltpu.CompilerParams(
            collective_id=0, has_side_effects=True, vmem_limit_bytes=60 * 1024 * 1024
        ),
        name="layer",
    )(
        hidden_in,
        mix_gain.reshape(1, D),
        jnp.transpose(w_gates, (0, 2, 1)),
        gate_bias,
        state_norm,
        state_max.T,
        ffn_gain.reshape(1, D),
        routes.T,
        route_weights.T,
        *big,
    )
    new_matrix = forget.T[:, :, None, None] * state_matrix + iv[..., :, None] * kk[..., None, :]
    return (result, new_matrix, new_norm, new_max.T)


def solution(mesh):
    placed = (
        P("ep", None),
        P(),
        P("ep", "tp"),
        P("ep", "tp"),
        P("ep", "tp"),
        P("ep", "tp"),
        P(None, None, "tp"),
        P(None, "tp"),
        P("ep", "tp", None, None),
        P("ep", "tp", None),
        P("ep", "tp"),
        P("tp", None),
        P(),
        P(),
        P("ep", None),
        P("ep", None, "tp"),
        P("ep", None, "tp"),
        P("ep", "tp", None),
        P(None, "tp"),
        P(None, "tp"),
        P("tp", None),
    )
    return jax.shard_map(
        per_device,
        mesh=mesh,
        in_specs=placed,
        out_specs=(P("ep", "tp"), P("ep", "tp", None, None), P("ep", "tp", None), P("ep", "tp")),
        check_vma=False,
    )
```

```python
import functools

import jax
import jax.numpy as jnp
from jax import lax
from jax.experimental import pallas as pl
from jax.experimental.pallas import tpu as pltpu
from jax.sharding import PartitionSpec as P

norm_eps = 1e-06
F32 = jnp.float32
BF16 = jnp.bfloat16
MESH = pl.DeviceIdType.MESH


def dot(a, b):
    return jnp.dot(a, b, preferred_element_type=F32)


def flipped(index, mask):
    out, bit = index, 1
    while bit <= mask:
        if mask & bit:
            out = out + bit * (1 - 2 * lax.rem(lax.div(index, bit), 2))
        bit *= 2
    return out


def partners(index, count):
    if count & (count - 1) == 0:
        return [(flipped(index, m), flipped(index, m)) for m in range(1, count)]
    return [(lax.rem(index + d, count), lax.rem(index + count - d, count)) for d in range(1, count)]


def memory_kernel(
    result_in, norm_in, max_in, forget, iv, kk, state_hbm, result, matrix_hbm, norm, new_max,
    state, matrix, in_sem, out_sem,
):
    pieces, size, heads = state.shape[:3]
    ins, outs = [], []
    for n in range(pieces):
        span = pl.ds(n * size, size)
        ins.append(pltpu.make_async_copy(state_hbm.at[span], state.at[n], in_sem.at[n]))
        outs.append(pltpu.make_async_copy(matrix.at[n], matrix_hbm.at[span], out_sem.at[n]))
        ins[n].start()
    result[...] = result_in[...]
    norm[...] = norm_in[...]
    new_max[...] = max_in[...]
    for n in range(pieces):
        ins[n].wait()
        for m in range(size):
            s = n * size + m
            for h in range(heads):
                matrix[n, m, h] = forget[h, s] * state[n, m, h] + iv[h, :, s : s + 1] * kk[s, h : h + 1, :]
        outs[n].start()
    for copy in outs:
        copy.wait()


def layer_kernel(
    dims,
    hidden_ref,
    mix_gain_ref,
    w_gates_ref,
    bias_ref,
    norm_ref,
    max_ref,
    ffn_gain_ref,
    routes_ref,
    weights_ref,
    wq_hbm,
    wk_hbm,
    wv_hbm,
    wo_hbm,
    state_hbm,
    mix_hbm,
    sg_hbm,
    su_hbm,
    sd_hbm,
    eg_hbm,
    eu_hbm,
    ed_hbm,
    result_ref,
    new_max_ref,
    new_norm_ref,
    forget_ref,
    iv_ref,
    kk_ref,
    wq,
    wk,
    wv,
    wo,
    state,
    mix,
    sg,
    su,
    sd,
    eg,
    eu,
    ed,
    normed,
    gathered,
    part,
    proj_in,
    q_heads,
    pads,
    routes_t,
    mix_out,
    mix_in,
    mix_own,
    zs,
    zr,
    half,
    other,
    sel,
    rx_a,
    rx_b,
    x_shared,
    sh_out,
    sh_in,
    sh_own,
    x_rows,
    hid,
    pair_out,
    pair_in,
    pair_own,
    ret_out,
    ret_in,
    comb,
    zs2,
    zr2,
    turn,
    local_sem,
    send_sem,
    recv_sem,
):
    E, T, S, D, H, hd, Le, cap, pad_rows, top = dims
    Z = T // 2
    SW = D // T
    Dk = D // E
    rows = Le * cap
    g = lax.axis_index("ep")
    t = lax.axis_index("tp")
    z = lax.div(t, 2)
    c = lax.rem(t, 2)
    partner = {"tp": t + 1 - 2 * c}
    locals_ = []
    early = 4
    for n, (src, dst) in enumerate(
        zip(
            (wq_hbm, wk_hbm, wv_hbm, wo_hbm, state_hbm, mix_hbm, sg_hbm, su_hbm, sd_hbm, eg_hbm, eu_hbm, ed_hbm),
            (wq, wk, wv, wo, state, mix, sg, su, sd, eg, eu, ed),
        )
    ):
        locals_.append(pltpu.make_async_copy(src, dst, local_sem.at[n]))
    for copy in locals_[:early]:
        copy.start()

    barrier = pltpu.get_barrier_semaphore()
    lo = rows // 16 * 16
    if lo < pad_rows:
        for buf in (rx_a, rx_b, ret_in):
            buf[:, :, lo:, :] = jnp.zeros((Z, E, pad_rows - lo, SW), BF16)
    ep_peers = partners(g, E)
    z_peers = partners(z, Z)
    pl.semaphore_signal(barrier, inc=1, device_id=partner, device_id_type=MESH)
    for to, _ in z_peers:
        pl.semaphore_signal(barrier, inc=1, device_id={"tp": to * 2 + c}, device_id_type=MESH)
    for to, _ in ep_peers:
        pl.semaphore_signal(barrier, inc=1, device_id={"ep": to}, device_id_type=MESH)

    sent = []

    def remote(src, dst, device):
        n = len(sent)
        copy = pltpu.make_async_remote_copy(
            src_ref=src,
            dst_ref=dst,
            send_sem=send_sem.at[n],
            recv_sem=recv_sem.at[n],
            device_id=device,
            device_id_type=MESH,
        )
        copy.start()
        sent.append(copy)
        return copy

    def columns(zi, core):
        return pl.ds(pl.multiple_of((zi * 2 + core) * SW, SW), SW)

    def transposed(slot, value):
        pads[slot] = jnp.zeros((8, 128), F32)
        pads[slot, : value.shape[0], : value.shape[1]] = value
        return pads[slot].T

    floats = hidden_ref[...].astype(F32)
    scale = lax.rsqrt(jnp.mean(floats * floats, -1, keepdims=True) + norm_eps)
    for p in range(E):
        span = slice(p * Dk, (p + 1) * Dk)
        normed[p] = (hidden_ref[:, span].astype(F32) * scale * mix_gain_ref[:, span]).astype(BF16)
    pl.semaphore_wait(barrier, Z + E - 1)
    moves = [remote(normed.at[to], gathered.at[g], {"ep": to}) for to, _ in ep_peers]
    for copy in locals_[early:]:
        copy.start()

    bias_t = transposed(0, bias_ref[...])
    gate_pre = []
    for role in range(2):
        total = jnp.zeros((H, S), F32)
        for p in range(E):
            total = total + lax.dot_general(
                w_gates_ref[role, :, p * Dk : (p + 1) * Dk],
                normed[p],
                (((1,), (1,)), ((), ())),
                preferred_element_type=F32,
            )
        gate_pre.append(total + bias_t[:H, role : role + 1])
    carried = jnp.minimum(gate_pre[1], 0.0) - jnp.log(1.0 + jnp.exp(-jnp.abs(gate_pre[1]))) + max_ref[...]
    new_max = jnp.maximum(carried, gate_pre[0])
    forget = jnp.exp(carried - new_max)
    take = jnp.exp(gate_pre[0] - new_max)
    new_max_ref[...] = new_max
    forget_ref[...] = forget
    forget_t = transposed(1, forget)
    take_t = transposed(2, take)

    route_floats = routes_ref[...].astype(F32)
    routes_t[...] = jnp.concatenate(
        [route_floats, jnp.zeros((8 - top, route_floats.shape[1]), F32)], 0
    ).T
    own_routes = routes_t[pl.ds(pl.multiple_of(g * S, 8), S), :]
    weights_t = transposed(3, weights_ref[...])
    lane = lax.broadcasted_iota(jnp.int32, (S, 128), 1).astype(F32)
    named = [(own_routes[:, k : k + 1] == lane).astype(F32) for k in range(top)]
    onehot = functools.reduce(jnp.add, named)
    earlier = (
        lax.broadcasted_iota(jnp.int32, (S, S), 0) > lax.broadcasted_iota(jnp.int32, (S, S), 1)
    ).astype(F32)
    rank = dot(earlier.astype(BF16), onehot.astype(BF16))
    owner = jnp.floor((lane + 0.5) / Le)
    base = rank + owner * pad_rows + (lane - owner * Le) * cap
    slot_lane = lax.broadcasted_iota(jnp.int32, (S, E * pad_rows), 1).astype(F32)
    match = jnp.zeros((S, E * pad_rows), F32)
    share = jnp.zeros((S, E * pad_rows), F32)
    for k in range(top):
        slot = jnp.sum(base * named[k], -1, keepdims=True)
        hit = slot_lane == slot
        match = jnp.where(hit, 1.0, match)
        share = jnp.where(hit, weights_t[:S, k : k + 1], share)
    chooser = match.T.astype(BF16)
    share_hi = share.astype(BF16)
    share_lo = (share - share_hi.astype(F32)).astype(BF16)

    for n in range(4):
        locals_[n].wait()
    hc = H * hd

    def project(block):
        return jnp.concatenate([dot(block, w[...]) for w in (wq, wk, wv, wo)], -1)

    projected = project(normed[g])
    back_moves = []
    for move, (_, source) in zip(moves, ep_peers):
        move.wait_recv()
        part[source] = project(gathered[source]).astype(BF16)
        back_moves.append(remote(part.at[source], proj_in.at[g], {"ep": source}))
    locals_[4].wait()
    for move, (source, _) in zip(back_moves, ep_peers):
        move.wait_recv()
        projected = projected + proj_in[source].astype(F32)
    projected = projected.astype(BF16).astype(F32)

    for h in range(H):
        q_heads[h] = projected[:, h * hd : (h + 1) * hd]
    lane64 = lax.broadcasted_iota(jnp.int32, (hd, 128), 1)

    def read_row(s, totals):
        out = []
        for h in range(H):
            product = state[s, h] * q_heads[h, pl.ds(s, 1), :]
            out.append(jnp.where(lane64 == s, jnp.sum(product, -1, keepdims=True), totals[h]))
        return tuple(out)

    reads = lax.fori_loop(0, S, read_row, tuple(jnp.zeros((hd, 128), F32) for _ in range(H)))
    gated = []
    for h in range(H):
        query = q_heads[h]
        key = projected[:, hc + h * hd : hc + (h + 1) * hd] * hd ** (-0.5)
        value = projected[:, 2 * hc + h * hd : 2 * hc + (h + 1) * hd]
        gate = projected[:, 3 * hc + h * hd : 3 * hc + (h + 1) * hd]
        keep = forget_t[:S, h : h + 1]
        put = take_t[:S, h : h + 1]
        put_value = put * value
        new_norm = keep * norm_ref[:, h, :] + put * key
        new_norm_ref[:, h, :] = new_norm
        turn[:, :hd] = put_value
        iv_ref[h] = turn[...].T[:hd, :]
        kk_ref[:, h, :] = key
        numerator = keep * reads[h].T[:S, :] + put_value * jnp.sum(key * query, -1, keepdims=True)
        denominator = jnp.maximum(jnp.abs(jnp.sum(new_norm * query, -1, keepdims=True)), 1.0)
        gated.append(numerator / (denominator * (1.0 + jnp.exp(-gate))))
    gated = jnp.concatenate(gated, -1).astype(BF16)

    locals_[5].wait()
    far_first = z_peers[::-1]
    chunks = [to for to, _ in far_first] + [z]
    pair_moves = []
    for to in chunks:
        mix_out[to] = dot(gated, mix[:, columns(to, 1 - c)]).astype(BF16)
        pair_moves.append(remote(mix_out.at[to], mix_in.at[to], partner))
    moves = []
    for n, to in enumerate(chunks):
        own = dot(gated, mix[:, columns(to, c)])
        pair_moves[n].wait_recv()
        own = own + mix_in[to].astype(F32)
        if n < Z - 1:
            zs[to] = own.astype(BF16)
            moves.append(remote(zs.at[to], zr.at[z], {"tp": to * 2 + c}))
        else:
            mixed = own + hidden_ref[:, columns(z, c)].astype(F32)
    for move, (_, source) in zip(moves, far_first):
        move.wait_recv()
        mixed = mixed + zr[source].astype(F32)
    stream_own = mixed.astype(BF16)

    kept = pl.ds(0, -(-rows // 8) * 8)
    row_moves = []
    row_shares = []

    def select(chunk):
        sel[chunk] = dot(chooser, half[chunk]).astype(BF16).reshape(E, pad_rows, SW)
        for to, source in ep_peers[::-1]:
            move = remote(sel.at[chunk, to, kept], rx_a.at[chunk, g, kept], {"ep": to})
            row_moves.append((move, chunk, source))
        row_shares.append(remote(sel.at[chunk, g, kept], rx_b.at[chunk, g, kept], partner))
        rx_a[chunk, g] = sel[chunk, g]

    def hand_over(entries):
        for move, chunk, source in entries:
            move.wait_recv()
            row_shares.append(
                remote(rx_a.at[chunk, source, kept], rx_b.at[chunk, source, kept], partner)
            )

    half[z] = stream_own
    moves = [remote(half.at[z], half.at[z], {"tp": to * 2 + c}) for to, _ in far_first][::-1]
    shares = [remote(half.at[z], other.at[z], partner)]
    select(z)
    for move, (_, source) in zip(moves, z_peers):
        move.wait_recv()
        shares.append(remote(half.at[source], other.at[source], partner))
        select(source)
    hand_over(row_moves[: 2 * (E - 1)])

    for move in shares:
        move.wait_recv()
    squares = jnp.zeros((S, 1), F32)
    for zi in range(Z):
        for buf in (half, other):
            floats = buf[zi].astype(F32)
            squares = squares + jnp.sum(floats * floats, -1, keepdims=True)
    scale = lax.rsqrt(squares / D + norm_eps)
    for zi in range(Z):
        for buf, core in ((half, c), (other, 1 - c)):
            span = columns(zi, core)
            x_shared[:, span] = (buf[zi].astype(F32) * scale * ffn_gain_ref[:, span]).astype(BF16)
    for n in range(6, 9):
        locals_[n].wait()
    inputs = x_shared[...]
    gate = dot(inputs, sg[...])
    shared_hidden = (gate / (1.0 + jnp.exp(-gate)) * dot(inputs, su[...])).astype(BF16)
    hand_over(row_moves[2 * (E - 1) :])
    shared_moves = []
    for zi in range(Z):
        sh_out[zi] = dot(shared_hidden, sd[:, columns(zi, 1 - c)]).astype(BF16)
        shared_moves.append(remote(sh_out.at[zi], sh_in.at[zi], partner))
    for zi in range(Z):
        sh_own[zi] = dot(shared_hidden, sd[:, columns(zi, c)])

    for move in row_shares:
        move.wait_recv()
    count = E * pad_rows
    squares = jnp.zeros((count, 1), F32)
    for buf in (rx_a, rx_b):
        for zi in range(Z):
            floats = buf[zi].reshape(count, SW).astype(F32)
            squares = squares + jnp.sum(floats * floats, -1, keepdims=True)
    scale = lax.rsqrt(squares / D + norm_eps)
    for zi in range(Z):
        for buf, core in ((rx_a, c), (rx_b, 1 - c)):
            span = columns(zi, core)
            floats = buf[zi].reshape(count, SW).astype(F32)
            x_rows[:, span] = (floats * scale * ffn_gain_ref[:, span]).astype(BF16)
    for n in range(9, 12):
        locals_[n].wait()
    width = eg.shape[2]
    place = lax.broadcasted_iota(jnp.int32, (E, pad_rows, width), 1).reshape(count, width)
    for e in range(Le):
        gate = dot(x_rows[...], eg[e])
        value = gate / (1.0 + jnp.exp(-gate)) * dot(x_rows[...], eu[e])
        value = jnp.where((place >= e * cap) & (place < (e + 1) * cap), value, 0.0)
        hid[:, e * width : (e + 1) * width] = value.astype(BF16)
    pair_moves = []
    for to in chunks:
        pair_out[to] = dot(hid[...], ed[:, columns(to, 1 - c)]).astype(BF16)
        pair_moves.append(remote(pair_out.at[to], pair_in.at[to], partner))
    ret_moves = []
    for n, chunk in enumerate(chunks):
        own = dot(hid[...], ed[:, columns(chunk, c)])
        pair_moves[n].wait_recv()
        both = own + pair_in[chunk].astype(F32)
        ret_out[chunk] = both.astype(BF16).reshape(E, pad_rows, SW)
        ret_moves.append(
            [
                remote(ret_out.at[chunk, to, kept], ret_in.at[chunk, g, kept], {"ep": to})
                for to, _ in ep_peers[::-1]
            ]
        )
        ret_in[chunk, g] = ret_out[chunk, g]
    for move in shared_moves:
        move.wait_recv()

    moves = []
    for n, chunk in enumerate(chunks):
        for move in ret_moves[n]:
            move.wait_recv()
        back = ret_in[chunk].reshape(count, SW)
        own = dot(share_hi, back) + dot(share_lo, back) + sh_own[chunk] + sh_in[chunk].astype(F32)
        if n < Z - 1:
            zs2[chunk] = own.astype(BF16)
            moves.append(remote(zs2.at[chunk], zr2.at[z], {"tp": chunk * 2 + c}))
        else:
            total = half[z].astype(F32) + own
    for move, (_, source) in zip(moves, far_first):
        move.wait_recv()
        total = total + zr2[source].astype(F32)
    result_ref[...] = total.astype(BF16)
    for copy in sent:
        copy.wait_send()


def per_device(
    hidden_in,
    mix_gain,
    w_query,
    w_key,
    w_value,
    w_outgate,
    w_gates,
    gate_bias,
    state_matrix,
    state_norm,
    state_max,
    w_mix_out,
    ffn_gain,
    routes,
    route_weights,
    expert_gate,
    expert_up,
    expert_down,
    shared_gate,
    shared_up,
    shared_down,
):
    E = lax.axis_size("ep")
    T = lax.axis_size("tp")
    S, D = hidden_in.shape
    H, hd = state_matrix.shape[1:3]
    top = routes.shape[1]
    Le, _, width = expert_gate.shape
    cap = max(2, S * top // (Le * E) + 1)
    pad_rows = -(-Le * cap // 16) * 16
    Z, SW, Dk, count = T // 2, D // T, D // E, E * pad_rows
    batch = routes.shape[0]
    dims = (E, T, S, D, H, hd, Le, cap, pad_rows, top)
    vmem = pl.BlockSpec(memory_space=pltpu.VMEM)
    hbm = pl.BlockSpec(memory_space=pl.ANY)
    down = expert_down.reshape(Le * width, D)
    big = (
        w_query, w_key, w_value, w_outgate, state_matrix, w_mix_out,
        shared_gate, shared_up, shared_down, expert_gate, expert_up, down,
    )
    V = pltpu.VMEM
    sems = (2 + 3 * Z) * E + 10 * Z + 8
    result, new_max, new_norm, forget, iv, kk = pl.pallas_call(
        functools.partial(layer_kernel, dims),
        out_shape=(
            jax.ShapeDtypeStruct((S, SW), BF16),
            jax.ShapeDtypeStruct((H, S), F32),
            jax.ShapeDtypeStruct((S, H, hd), F32),
            jax.ShapeDtypeStruct((H, S), F32),
            jax.ShapeDtypeStruct((H, hd, S), F32),
            jax.ShapeDtypeStruct((S, H, hd), F32),
        ),
        in_specs=[vmem] * 9 + [hbm] * len(big),
        out_specs=(vmem,) * 6,
        scratch_shapes=[V(a.shape, a.dtype) for a in big]
        + [
            V((E, S, Dk), BF16),
            V((E, S, Dk), BF16),
            V((E, S, 4 * H * hd), BF16),
            V((E, S, 4 * H * hd), BF16),
            V((H, S, hd), F32),
            V((4, 8, 128), F32),
            V((batch, 8), F32),
            V((Z, S, SW), BF16),
            V((Z, S, SW), BF16),
            V((Z, S, SW), F32),
            V((Z, S, SW), BF16),
            V((Z, S, SW), BF16),
            V((Z, S, SW), BF16),
            V((Z, S, SW), BF16),
            V((Z, E, pad_rows, SW), BF16),
            V((Z, E, pad_rows, SW), BF16),
            V((Z, E, pad_rows, SW), BF16),
            V((S, D), BF16),
            V((Z, S, SW), BF16),
            V((Z, S, SW), BF16),
            V((Z, S, SW), F32),
            V((count, D), BF16),
            V((count, Le * width), BF16),
            V((Z, count, SW), BF16),
            V((Z, count, SW), BF16),
            V((Z, count, SW), F32),
            V((Z, E, pad_rows, SW), BF16),
            V((Z, E, pad_rows, SW), BF16),
            V((Z, S, SW), F32),
            V((Z, S, SW), BF16),
            V((Z, S, SW), BF16),
            V((S, 128), F32),
            pltpu.SemaphoreType.DMA((len(big),)),
            pltpu.SemaphoreType.DMA((sems,)),
            pltpu.SemaphoreType.DMA((sems,)),
        ],
        compiler_params=pltpu.CompilerParams(
            collective_id=0, has_side_effects=True, vmem_limit_bytes=60 * 1024 * 1024
        ),
        name="layer",
    )(
        hidden_in,
        mix_gain.reshape(1, D),
        jnp.transpose(w_gates, (0, 2, 1)),
        gate_bias,
        state_norm,
        state_max.T,
        ffn_gain.reshape(1, D),
        routes.T,
        route_weights.T,
        *big,
    )
    pieces = 4 if S % 4 == 0 else 1
    held = (pieces, S // pieces, H, hd, hd)
    result, new_matrix, new_norm, new_max = pl.pallas_call(
        memory_kernel,
        out_shape=(
            jax.ShapeDtypeStruct((S, SW), BF16),
            jax.ShapeDtypeStruct(state_matrix.shape, F32),
            jax.ShapeDtypeStruct((S, H, hd), F32),
            jax.ShapeDtypeStruct((H, S), F32),
        ),
        in_specs=[vmem] * 3 + [pl.BlockSpec(memory_space=pltpu.SMEM)] + [vmem] * 2 + [hbm],
        out_specs=(vmem, hbm, vmem, vmem),
        scratch_shapes=[
            V(held, F32),
            V(held, F32),
            pltpu.SemaphoreType.DMA((pieces,)),
            pltpu.SemaphoreType.DMA((pieces,)),
        ],
        compiler_params=pltpu.CompilerParams(vmem_limit_bytes=40 * 1024 * 1024),
        name="memory",
    )(result, new_norm, new_max, forget, iv, kk, state_matrix)
    return (result, new_matrix, new_norm, new_max.T)


def solution(mesh):
    placed = (
        P("ep", None),
        P(),
        P("ep", "tp"),
        P("ep", "tp"),
        P("ep", "tp"),
        P("ep", "tp"),
        P(None, None, "tp"),
        P(None, "tp"),
        P("ep", "tp", None, None),
        P("ep", "tp", None),
        P("ep", "tp"),
        P("tp", None),
        P(),
        P(),
        P("ep", None),
        P("ep", None, "tp"),
        P("ep", None, "tp"),
        P("ep", "tp", None),
        P(None, "tp"),
        P(None, "tp"),
        P("tp", None),
    )
    return jax.shard_map(
        per_device,
        mesh=mesh,
        in_specs=placed,
        out_specs=(P("ep", "tp"), P("ep", "tp", None, None), P("ep", "tp", None), P("ep", "tp")),
        check_vma=False,
    )
```

```python
import functools

import jax
import jax.numpy as jnp
from jax import lax
from jax.experimental import pallas as pl
from jax.experimental.pallas import tpu as pltpu
from jax.sharding import PartitionSpec as P

norm_eps = 1e-06
F32 = jnp.float32
BF16 = jnp.bfloat16
MESH = pl.DeviceIdType.MESH


def dot(a, b):
    return jnp.dot(a, b, preferred_element_type=F32)


def flipped(index, mask):
    out, bit = index, 1
    while bit <= mask:
        if mask & bit:
            out = out + bit * (1 - 2 * lax.rem(lax.div(index, bit), 2))
        bit *= 2
    return out


def partners(index, count):
    if count & (count - 1) == 0:
        return [(flipped(index, m), flipped(index, m)) for m in range(1, count)]
    return [(lax.rem(index + d, count), lax.rem(index + count - d, count)) for d in range(1, count)]


def memory_kernel(
    result_in, norm_in, max_in, forget, iv, kk, state_hbm, result, matrix_hbm, norm, new_max,
    state, matrix, in_sem, out_sem,
):
    pieces, size, heads = state.shape[:3]
    ins, outs = [], []
    for n in range(pieces):
        span = pl.ds(n * size, size)
        ins.append(pltpu.make_async_copy(state_hbm.at[span], state.at[n], in_sem.at[n]))
        outs.append(pltpu.make_async_copy(matrix.at[n], matrix_hbm.at[span], out_sem.at[n]))
        ins[n].start()
    result[...] = result_in[...]
    norm[...] = norm_in[...]
    new_max[...] = max_in[...]
    for n in range(pieces):
        ins[n].wait()
        for m in range(size):
            s = n * size + m
            for h in range(heads):
                matrix[n, m, h] = forget[h, s] * state[n, m, h] + iv[h, :, s : s + 1] * kk[s, h : h + 1, :]
        outs[n].start()
    for copy in outs:
        copy.wait()


def layer_kernel(
    dims,
    hidden_ref,
    mix_gain_ref,
    w_gates_ref,
    bias_ref,
    norm_ref,
    max_ref,
    ffn_gain_ref,
    routes_ref,
    weights_ref,
    wq_hbm,
    wk_hbm,
    wv_hbm,
    wo_hbm,
    state_hbm,
    mix_hbm,
    sg_hbm,
    su_hbm,
    sd_hbm,
    eg_hbm,
    eu_hbm,
    ed_hbm,
    result_ref,
    new_max_ref,
    new_norm_ref,
    forget_ref,
    iv_ref,
    kk_ref,
    wq,
    wk,
    wv,
    wo,
    state,
    mix,
    sg,
    su,
    sd,
    eg,
    eu,
    ed,
    normed,
    gathered,
    part,
    proj_in,
    q_heads,
    pads,
    routes_t,
    mix_out,
    mix_in,
    mix_own,
    zs,
    zr,
    half,
    other,
    sel,
    rx_a,
    rx_b,
    x_shared,
    sh_out,
    sh_in,
    sh_own,
    x_rows,
    hid,
    pair_out,
    pair_in,
    pair_own,
    ret_out,
    ret_in,
    comb,
    zs2,
    zr2,
    turn,
    local_sem,
    send_sem,
    recv_sem,
):
    E, T, S, D, H, hd, Le, cap, pad_rows, top = dims
    Z = T // 2
    SW = D // T
    Dk = D // E
    rows = Le * cap
    g = lax.axis_index("ep")
    t = lax.axis_index("tp")
    z = lax.div(t, 2)
    c = lax.rem(t, 2)
    partner = {"tp": t + 1 - 2 * c}
    locals_ = []
    early = 4
    for n, (src, dst) in enumerate(
        zip(
            (wq_hbm, wk_hbm, wv_hbm, wo_hbm, state_hbm, mix_hbm, sg_hbm, su_hbm, sd_hbm, eg_hbm, eu_hbm, ed_hbm),
            (wq, wk, wv, wo, state, mix, sg, su, sd, eg, eu, ed),
        )
    ):
        locals_.append(pltpu.make_async_copy(src, dst, local_sem.at[n]))
    for copy in locals_[:early]:
        copy.start()

    barrier = pltpu.get_barrier_semaphore()
    lo = rows // 16 * 16
    if lo < pad_rows:
        for buf in (rx_a, rx_b, ret_in):
            buf[:, :, lo:, :] = jnp.zeros((Z, E, pad_rows - lo, SW), BF16)
    ep_peers = partners(g, E)
    z_peers = partners(z, Z)
    pl.semaphore_signal(barrier, inc=1, device_id=partner, device_id_type=MESH)
    for to, _ in z_peers:
        pl.semaphore_signal(barrier, inc=1, device_id={"tp": to * 2 + c}, device_id_type=MESH)
    for to, _ in ep_peers:
        pl.semaphore_signal(barrier, inc=1, device_id={"ep": to}, device_id_type=MESH)

    sent = []

    def remote(src, dst, device):
        n = len(sent)
        copy = pltpu.make_async_remote_copy(
            src_ref=src,
            dst_ref=dst,
            send_sem=send_sem.at[n],
            recv_sem=recv_sem.at[n],
            device_id=device,
            device_id_type=MESH,
        )
        copy.start()
        sent.append(copy)
        return copy

    def columns(zi, core):
        return pl.ds(pl.multiple_of((zi * 2 + core) * SW, SW), SW)

    def transposed(slot, value):
        pads[slot] = jnp.zeros((8, 128), F32)
        pads[slot, : value.shape[0], : value.shape[1]] = value
        return pads[slot].T

    floats = hidden_ref[...].astype(F32)
    scale = lax.rsqrt(jnp.mean(floats * floats, -1, keepdims=True) + norm_eps)
    for p in range(E):
        span = slice(p * Dk, (p + 1) * Dk)
        normed[p] = (hidden_ref[:, span].astype(F32) * scale * mix_gain_ref[:, span]).astype(BF16)
    pl.semaphore_wait(barrier, Z + E - 1)
    moves = [remote(normed.at[to], gathered.at[g], {"ep": to}) for to, _ in ep_peers]
    for copy in locals_[early:]:
        copy.start()

    bias_t = transposed(0, bias_ref[...])
    gate_pre = []
    for role in range(2):
        total = jnp.zeros((H, S), F32)
        for p in range(E):
            total = total + lax.dot_general(
                w_gates_ref[role, :, p * Dk : (p + 1) * Dk],
                normed[p],
                (((1,), (1,)), ((), ())),
                preferred_element_type=F32,
            )
        gate_pre.append(total + bias_t[:H, role : role + 1])
    carried = jnp.minimum(gate_pre[1], 0.0) - jnp.log(1.0 + jnp.exp(-jnp.abs(gate_pre[1]))) + max_ref[...]
    new_max = jnp.maximum(carried, gate_pre[0])
    forget = jnp.exp(carried - new_max)
    take = jnp.exp(gate_pre[0] - new_max)
    new_max_ref[...] = new_max
    forget_ref[...] = forget
    forget_t = transposed(1, forget)
    take_t = transposed(2, take)

    route_floats = routes_ref[...].astype(F32)
    routes_t[...] = jnp.concatenate(
        [route_floats, jnp.zeros((8 - top, route_floats.shape[1]), F32)], 0
    ).T
    own_routes = routes_t[pl.ds(pl.multiple_of(g * S, 8), S), :]
    weights_t = transposed(3, weights_ref[...])
    lane = lax.broadcasted_iota(jnp.int32, (S, 128), 1).astype(F32)
    named = [(own_routes[:, k : k + 1] == lane).astype(F32) for k in range(top)]
    onehot = functools.reduce(jnp.add, named)
    earlier = (
        lax.broadcasted_iota(jnp.int32, (S, S), 0) > lax.broadcasted_iota(jnp.int32, (S, S), 1)
    ).astype(F32)
    rank = dot(earlier.astype(BF16), onehot.astype(BF16))
    owner = jnp.floor((lane + 0.5) / Le)
    base = rank + owner * pad_rows + (lane - owner * Le) * cap
    slot_lane = lax.broadcasted_iota(jnp.int32, (S, E * pad_rows), 1).astype(F32)
    match = jnp.zeros((S, E * pad_rows), F32)
    share = jnp.zeros((S, E * pad_rows), F32)
    for k in range(top):
        slot = jnp.sum(base * named[k], -1, keepdims=True)
        hit = slot_lane == slot
        match = jnp.where(hit, 1.0, match)
        share = jnp.where(hit, weights_t[:S, k : k + 1], share)
    chooser = match.T.astype(BF16)
    share_hi = share.astype(BF16)
    share_lo = (share - share_hi.astype(F32)).astype(BF16)

    for n in range(4):
        locals_[n].wait()
    hc = H * hd

    def project(block):
        return jnp.concatenate([dot(block, w[...]) for w in (wq, wk, wv, wo)], -1)

    projected = project(normed[g])
    back_moves = []
    for move, (_, source) in zip(moves, ep_peers):
        move.wait_recv()
        part[source] = project(gathered[source]).astype(BF16)
        back_moves.append(remote(part.at[source], proj_in.at[g], {"ep": source}))
    locals_[4].wait()
    for move, (source, _) in zip(back_moves, ep_peers):
        move.wait_recv()
        projected = projected + proj_in[source].astype(F32)
    projected = projected.astype(BF16).astype(F32)

    for h in range(H):
        q_heads[h] = projected[:, h * hd : (h + 1) * hd]
    lane64 = lax.broadcasted_iota(jnp.int32, (hd, 128), 1)

    def read_row(s, totals):
        out = []
        for h in range(H):
            product = state[s, h] * q_heads[h, pl.ds(s, 1), :]
            out.append(jnp.where(lane64 == s, jnp.sum(product, -1, keepdims=True), totals[h]))
        return tuple(out)

    reads = lax.fori_loop(0, S, read_row, tuple(jnp.zeros((hd, 128), F32) for _ in range(H)))
    gated = []
    for h in range(H):
        query = q_heads[h]
        key = projected[:, hc + h * hd : hc + (h + 1) * hd] * hd ** (-0.5)
        value = projected[:, 2 * hc + h * hd : 2 * hc + (h + 1) * hd]
        gate = projected[:, 3 * hc + h * hd : 3 * hc + (h + 1) * hd]
        keep = forget_t[:S, h : h + 1]
        put = take_t[:S, h : h + 1]
        put_value = put * value
        new_norm = keep * norm_ref[:, h, :] + put * key
        new_norm_ref[:, h, :] = new_norm
        turn[:, :hd] = put_value
        iv_ref[h] = turn[...].T[:hd, :]
        kk_ref[:, h, :] = key
        numerator = keep * reads[h].T[:S, :] + put_value * jnp.sum(key * query, -1, keepdims=True)
        denominator = jnp.maximum(jnp.abs(jnp.sum(new_norm * query, -1, keepdims=True)), 1.0)
        gated.append(numerator / (denominator * (1.0 + jnp.exp(-gate))))
    gated = jnp.concatenate(gated, -1).astype(BF16)

    locals_[5].wait()
    far_first = z_peers[::-1]
    chunks = [to for to, _ in far_first] + [z]
    pair_moves = []
    for to in chunks:
        mix_out[to] = dot(gated, mix[:, columns(to, 1 - c)]).astype(BF16)
        pair_moves.append(remote(mix_out.at[to], mix_in.at[to], partner))
    moves = []
    for n, to in enumerate(chunks):
        own = dot(gated, mix[:, columns(to, c)])
        pair_moves[n].wait_recv()
        own = own + mix_in[to].astype(F32)
        if n < Z - 1:
            zs[to] = own.astype(BF16)
            moves.append(remote(zs.at[to], zr.at[z], {"tp": to * 2 + c}))
        else:
            mixed = own + hidden_ref[:, columns(z, c)].astype(F32)
    for move, (_, source) in zip(moves, far_first):
        move.wait_recv()
        mixed = mixed + zr[source].astype(F32)
    stream_own = mixed.astype(BF16)

    kept = pl.ds(0, -(-rows // 8) * 8)
    row_moves = []
    row_shares = []

    def select(chunk):
        sel[chunk] = dot(chooser, half[chunk]).astype(BF16).reshape(E, pad_rows, SW)
        for to, source in ep_peers[::-1]:
            move = remote(sel.at[chunk, to, kept], rx_a.at[chunk, g, kept], {"ep": to})
            row_moves.append((move, chunk, source))
        row_shares.append(remote(sel.at[chunk, g, kept], rx_b.at[chunk, g, kept], partner))
        rx_a[chunk, g] = sel[chunk, g]

    def hand_over(entries):
        for move, chunk, source in entries:
            move.wait_recv()
            row_shares.append(
                remote(rx_a.at[chunk, source, kept], rx_b.at[chunk, source, kept], partner)
            )

    half[z] = stream_own
    moves = [remote(half.at[z], half.at[z], {"tp": to * 2 + c}) for to, _ in far_first][::-1]
    shares = [remote(half.at[z], other.at[z], partner)]
    select(z)
    for move, (_, source) in zip(moves, z_peers):
        move.wait_recv()
        shares.append(remote(half.at[source], other.at[source], partner))
        select(source)
    hand_over(row_moves[: 2 * (E - 1)])

    hand_over(row_moves[2 * (E - 1) :])

    for move in row_shares:
        move.wait_recv()
    count = E * pad_rows
    squares = jnp.zeros((count, 1), F32)
    for buf in (rx_a, rx_b):
        for zi in range(Z):
            floats = buf[zi].reshape(count, SW).astype(F32)
            squares = squares + jnp.sum(floats * floats, -1, keepdims=True)
    scale = lax.rsqrt(squares / D + norm_eps)
    for zi in range(Z):
        for buf, core in ((rx_a, c), (rx_b, 1 - c)):
            span = columns(zi, core)
            floats = buf[zi].reshape(count, SW).astype(F32)
            x_rows[:, span] = (floats * scale * ffn_gain_ref[:, span]).astype(BF16)
    for n in range(9, 12):
        locals_[n].wait()
    width = eg.shape[2]
    place = lax.broadcasted_iota(jnp.int32, (E, pad_rows, width), 1).reshape(count, width)
    for e in range(Le):
        gate = dot(x_rows[...], eg[e])
        value = gate / (1.0 + jnp.exp(-gate)) * dot(x_rows[...], eu[e])
        value = jnp.where((place >= e * cap) & (place < (e + 1) * cap), value, 0.0)
        hid[:, e * width : (e + 1) * width] = value.astype(BF16)
    pair_moves = []
    for to in chunks:
        pair_out[to] = dot(hid[...], ed[:, columns(to, 1 - c)]).astype(BF16)
        pair_moves.append(remote(pair_out.at[to], pair_in.at[to], partner))
    ret_moves = []
    for n, chunk in enumerate(chunks):
        own = dot(hid[...], ed[:, columns(chunk, c)])
        pair_moves[n].wait_recv()
        both = own + pair_in[chunk].astype(F32)
        ret_out[chunk] = both.astype(BF16).reshape(E, pad_rows, SW)
        ret_moves.append(
            [
                remote(ret_out.at[chunk, to, kept], ret_in.at[chunk, g, kept], {"ep": to})
                for to, _ in ep_peers[::-1]
            ]
        )
        ret_in[chunk, g] = ret_out[chunk, g]

    for move in shares:
        move.wait_recv()
    squares = jnp.zeros((S, 1), F32)
    for zi in range(Z):
        for buf in (half, other):
            floats = buf[zi].astype(F32)
            squares = squares + jnp.sum(floats * floats, -1, keepdims=True)
    scale = lax.rsqrt(squares / D + norm_eps)
    for zi in range(Z):
        for buf, core in ((half, c), (other, 1 - c)):
            span = columns(zi, core)
            x_shared[:, span] = (buf[zi].astype(F32) * scale * ffn_gain_ref[:, span]).astype(BF16)
    for n in range(6, 9):
        locals_[n].wait()
    inputs = x_shared[...]
    gate = dot(inputs, sg[...])
    shared_hidden = (gate / (1.0 + jnp.exp(-gate)) * dot(inputs, su[...])).astype(BF16)
    shared_moves = []
    for zi in range(Z):
        sh_out[zi] = dot(shared_hidden, sd[:, columns(zi, 1 - c)]).astype(BF16)
        shared_moves.append(remote(sh_out.at[zi], sh_in.at[zi], partner))
    for zi in range(Z):
        sh_own[zi] = dot(shared_hidden, sd[:, columns(zi, c)])
    for move in shared_moves:
        move.wait_recv()

    moves = []
    for n, chunk in enumerate(chunks):
        for move in ret_moves[n]:
            move.wait_recv()
        back = ret_in[chunk].reshape(count, SW)
        own = dot(share_hi, back) + dot(share_lo, back) + sh_own[chunk] + sh_in[chunk].astype(F32)
        if n < Z - 1:
            zs2[chunk] = own.astype(BF16)
            moves.append(remote(zs2.at[chunk], zr2.at[z], {"tp": chunk * 2 + c}))
        else:
            total = half[z].astype(F32) + own
    for move, (_, source) in zip(moves, far_first):
        move.wait_recv()
        total = total + zr2[source].astype(F32)
    result_ref[...] = total.astype(BF16)
    for copy in sent:
        copy.wait_send()


def per_device(
    hidden_in,
    mix_gain,
    w_query,
    w_key,
    w_value,
    w_outgate,
    w_gates,
    gate_bias,
    state_matrix,
    state_norm,
    state_max,
    w_mix_out,
    ffn_gain,
    routes,
    route_weights,
    expert_gate,
    expert_up,
    expert_down,
    shared_gate,
    shared_up,
    shared_down,
):
    E = lax.axis_size("ep")
    T = lax.axis_size("tp")
    S, D = hidden_in.shape
    H, hd = state_matrix.shape[1:3]
    top = routes.shape[1]
    Le, _, width = expert_gate.shape
    cap = max(2, S * top // (Le * E) + 1)
    pad_rows = -(-Le * cap // 16) * 16
    Z, SW, Dk, count = T // 2, D // T, D // E, E * pad_rows
    batch = routes.shape[0]
    dims = (E, T, S, D, H, hd, Le, cap, pad_rows, top)
    vmem = pl.BlockSpec(memory_space=pltpu.VMEM)
    hbm = pl.BlockSpec(memory_space=pl.ANY)
    down = expert_down.reshape(Le * width, D)
    big = (
        w_query, w_key, w_value, w_outgate, state_matrix, w_mix_out,
        shared_gate, shared_up, shared_down, expert_gate, expert_up, down,
    )
    V = pltpu.VMEM
    sems = (2 + 3 * Z) * E + 10 * Z + 8
    result, new_max, new_norm, forget, iv, kk = pl.pallas_call(
        functools.partial(layer_kernel, dims),
        out_shape=(
            jax.ShapeDtypeStruct((S, SW), BF16),
            jax.ShapeDtypeStruct((H, S), F32),
            jax.ShapeDtypeStruct((S, H, hd), F32),
            jax.ShapeDtypeStruct((H, S), F32),
            jax.ShapeDtypeStruct((H, hd, S), F32),
            jax.ShapeDtypeStruct((S, H, hd), F32),
        ),
        in_specs=[vmem] * 9 + [hbm] * len(big),
        out_specs=(vmem,) * 6,
        scratch_shapes=[V(a.shape, a.dtype) for a in big]
        + [
            V((E, S, Dk), BF16),
            V((E, S, Dk), BF16),
            V((E, S, 4 * H * hd), BF16),
            V((E, S, 4 * H * hd), BF16),
            V((H, S, hd), F32),
            V((4, 8, 128), F32),
            V((batch, 8), F32),
            V((Z, S, SW), BF16),
            V((Z, S, SW), BF16),
            V((Z, S, SW), F32),
            V((Z, S, SW), BF16),
            V((Z, S, SW), BF16),
            V((Z, S, SW), BF16),
            V((Z, S, SW), BF16),
            V((Z, E, pad_rows, SW), BF16),
            V((Z, E, pad_rows, SW), BF16),
            V((Z, E, pad_rows, SW), BF16),
            V((S, D), BF16),
            V((Z, S, SW), BF16),
            V((Z, S, SW), BF16),
            V((Z, S, SW), F32),
            V((count, D), BF16),
            V((count, Le * width), BF16),
            V((Z, count, SW), BF16),
            V((Z, count, SW), BF16),
            V((Z, count, SW), F32),
            V((Z, E, pad_rows, SW), BF16),
            V((Z, E, pad_rows, SW), BF16),
            V((Z, S, SW), F32),
            V((Z, S, SW), BF16),
            V((Z, S, SW), BF16),
            V((S, 128), F32),
            pltpu.SemaphoreType.DMA((len(big),)),
            pltpu.SemaphoreType.DMA((sems,)),
            pltpu.SemaphoreType.DMA((sems,)),
        ],
        compiler_params=pltpu.CompilerParams(
            collective_id=0, has_side_effects=True, vmem_limit_bytes=60 * 1024 * 1024
        ),
        name="layer",
    )(
        hidden_in,
        mix_gain.reshape(1, D),
        jnp.transpose(w_gates, (0, 2, 1)),
        gate_bias,
        state_norm,
        state_max.T,
        ffn_gain.reshape(1, D),
        routes.T,
        route_weights.T,
        *big,
    )
    pieces = 4 if S % 4 == 0 else 1
    held = (pieces, S // pieces, H, hd, hd)
    result, new_matrix, new_norm, new_max = pl.pallas_call(
        memory_kernel,
        out_shape=(
            jax.ShapeDtypeStruct((S, SW), BF16),
            jax.ShapeDtypeStruct(state_matrix.shape, F32),
            jax.ShapeDtypeStruct((S, H, hd), F32),
            jax.ShapeDtypeStruct((H, S), F32),
        ),
        in_specs=[vmem] * 3 + [pl.BlockSpec(memory_space=pltpu.SMEM)] + [vmem] * 2 + [hbm],
        out_specs=(vmem, hbm, vmem, vmem),
        scratch_shapes=[
            V(held, F32),
            V(held, F32),
            pltpu.SemaphoreType.DMA((pieces,)),
            pltpu.SemaphoreType.DMA((pieces,)),
        ],
        compiler_params=pltpu.CompilerParams(vmem_limit_bytes=60 * 1024 * 1024),
        name="memory",
    )(result, new_norm, new_max, forget, iv, kk, state_matrix)
    return (result, new_matrix, new_norm, new_max.T)


def solution(mesh):
    placed = (
        P("ep", None),
        P(),
        P("ep", "tp"),
        P("ep", "tp"),
        P("ep", "tp"),
        P("ep", "tp"),
        P(None, None, "tp"),
        P(None, "tp"),
        P("ep", "tp", None, None),
        P("ep", "tp", None),
        P("ep", "tp"),
        P("tp", None),
        P(),
        P(),
        P("ep", None),
        P("ep", None, "tp"),
        P("ep", None, "tp"),
        P("ep", "tp", None),
        P(None, "tp"),
        P(None, "tp"),
        P("tp", None),
    )
    return jax.shard_map(
        per_device,
        mesh=mesh,
        in_specs=placed,
        out_specs=(P("ep", "tp"), P("ep", "tp", None, None), P("ep", "tp", None), P("ep", "tp")),
        check_vma=False,
    )
```
